32 devices in a mesh: sp: 16 (over z, y, x), tp: 2 (over core).
Axes of the slice: x: 2, y: 2, z: 4, core: 2. Of those that a mesh axis runs over, the one named last changes fastest.
Arguments:
- resid: bfloat16 [2048, 2048], P('sp'), may hold values from -6 to 6
- queries: bfloat16 [2048, 1024], P('sp', 'tp'), may hold values from -6 to 6
- keys: bfloat16 [2048, 1024], P('sp', 'tp'), may hold values from -6 to 6
- values: bfloat16 [2048, 2048], P('sp', 'tp'), may hold values from -6 to 6
- decay_pre: float32 [2048, 1024], P('sp', 'tp'), may hold values from -4 to 11.5
- out_gate: bfloat16 [2048, 2048], P('sp', 'tp'), may hold values from -6 to 6
- head_gain: float32 [256], replicated, may hold values from 0.1 to 1.9
- out_proj: bfloat16 [2048, 2048], P('tp'), may hold values from -0.25 to 0.25
- mix_gain: float32 [2048], replicated, may hold values from 0.1 to 1.9
- mix_shift: float32 [2048], replicated, may hold values from -3 to 3
- gate_in: bfloat16 [2048, 5632], P('sp', 'tp'), may hold values from -0.125 to 0.125
- up_in: bfloat16 [2048, 5632], P('sp', 'tp'), may hold values from -0.125 to 0.125
- down_out: bfloat16 [5632, 2048], P('tp', 'sp'), may hold values from -0.25 to 0.25
- out_gain: float32 [2048], replicated, may hold values from 0.1 to 1.9
- out_shift: float32 [2048], replicated, may hold values from -2 to 2
Outputs:
- result: bfloat16 [2048, 2048], P('sp')
The draws below stay inside these ranges and needn't reach their ends.
All inputs are finite; a program needn't handle non-finite values.
Results may differ from the reference program's by a relative error of at most 0.02.
Values may be sent and summed in bfloat16 or wider, within the bound.
A program may use at most 128 MiB of HBM per device.

```python
import jax
import jax.numpy as jnp
from jax import lax

D = 2048
HEADS = 8
HK = 128
HV = 256
FF = 5632
SPAN = 64
TOK_DEV = 128
TOKENS = 2048
KEYDIM = 1024
VALDIM = 2048
N_SP = 16
N_TP = 2


def draw_decay_pre(key, part):
    key_slow = jax.random.fold_in(key, 11)
    key_high = jax.random.fold_in(key, 12)
    key_low = jax.random.fold_in(key, 13)
    key_segment = jax.random.fold_in(key, 14)
    key_noise = jax.random.fold_in(key, 15)
    share = 0.5
    slow = jax.random.uniform(key_slow, (KEYDIM,), jnp.float32) < share
    keep_rate = jax.random.uniform(key_high, (KEYDIM,), jnp.float32, 0.5, 1.5)
    high = jnp.log(jnp.float32(TOKENS) / (16.0 * keep_rate))
    low = jax.random.uniform(key_low, (KEYDIM,), jnp.float32, -1.0, 1.0)
    base = jnp.where(slow, high, low)
    segment = jnp.arange(TOKENS) // TOK_DEV
    position_shifts = jax.random.uniform(key_segment, (TOKENS // TOK_DEV,), jnp.float32, -1.2, 1.2)[segment]
    noise = jnp.clip(jax.random.normal(key_noise, (TOKENS, KEYDIM), jnp.float32), -3.5, 3.5) * 0.5
    return (base[None, :] + position_shifts[:, None] + noise).astype(jnp.float32)


def shard_levels(rng, dims, shards, smallest, largest):
    loudness, own = 1.0, jax.random.fold_in(rng, 6)
    for dim, parts in shards:
        heights = jnp.exp(jax.random.uniform(jax.random.fold_in(own, dim), (parts,), jnp.float32, smallest / len(shards), largest / len(shards)))
        loudness = loudness * jnp.repeat(heights, dims[dim] // parts).reshape([-1 if axis == dim else 1 for axis in range(len(dims))])
    return loudness


def gaussian(own_key, dims, scale, most, shards=(), held_as=jnp.bfloat16):
    array = scale * jax.random.normal(own_key, dims, jnp.float32)
    if shards:
        array = array * shard_levels(own_key, dims, shards, -0.22, 0.18)
    return jnp.clip(array, -most, most).astype(held_as)


def setup_inputs(seed: int = 0) -> dict:
    arg_keys = jax.random.split(jax.random.key(seed), 16)
    resid = gaussian(arg_keys[0], (TOKENS, D), 1.0, 6.0, ((0, 16),))
    queries = gaussian(arg_keys[1], (TOKENS, KEYDIM), 1.0, 6.0, ((0, 16), (1, 2)))
    keys = gaussian(arg_keys[2], (TOKENS, KEYDIM), 1.0, 6.0, ((0, 16), (1, 2)))
    values = gaussian(arg_keys[3], (TOKENS, VALDIM), 1.0, 6.0, ((0, 16), (1, 2)))
    decay_pre = draw_decay_pre(jax.random.fold_in(arg_keys[15], 71), 0)
    out_gate = gaussian(arg_keys[5], (TOKENS, VALDIM), 1.0, 6.0, ((0, 16), (1, 2)))
    head_gain = jnp.clip(1.0 + 0.18 * jax.random.normal(arg_keys[6], (HV,), jnp.float32), 0.1, 1.9)
    out_proj = gaussian(arg_keys[7], (VALDIM, D), (VALDIM // 4) ** -0.5, 0.25, ((0, 2),))
    mix_gain = jnp.clip(1.0 + 0.18 * jax.random.normal(arg_keys[8], (D,), jnp.float32), 0.1, 1.9)
    mix_shift = gaussian(arg_keys[9], (D,), 0.5, 3.0, (), jnp.float32)
    gate_in = gaussian(arg_keys[10], (D, FF), D ** -0.5, 0.125, ((0, 16), (1, 2)))
    up_in = gaussian(arg_keys[11], (D, FF), D ** -0.5, 0.125, ((0, 16), (1, 2)))
    down_out = gaussian(arg_keys[12], (FF, D), (FF // 9) ** -0.5, 0.25, ((0, 2), (1, 16)))
    out_gain = jnp.clip(1.0 + 0.18 * jax.random.normal(arg_keys[13], (D,), jnp.float32), 0.1, 1.9)
    out_shift = gaussian(arg_keys[14], (D,), 0.3, 2.0, (), jnp.float32)
    return {"resid": resid, "queries": queries, "keys": keys, "values": values, "decay_pre": decay_pre, "out_gate": out_gate, "head_gain": head_gain, "out_proj": out_proj, "mix_gain": mix_gain, "mix_shift": mix_shift, "gate_in": gate_in, "up_in": up_in, "down_out": down_out, "out_gain": out_gain, "out_shift": out_shift}


ALPHA = 2.0 ** 0.25
LN_EPS = 1e-05
RMS_EPS = 1e-06
TAU = 16.0

def layer_norm(inputs, gain, shift):
    center = inputs - lax.optimization_barrier(jnp.mean(inputs, axis=-1, keepdims=True))
    spread = lax.optimization_barrier(jnp.mean(center * center, axis=-1, keepdims=True))
    return center * lax.rsqrt(spread + LN_EPS) * gain + shift

def group_sum(left, weight, width):
    total = jnp.zeros((left.shape[0], weight.shape[1]), jnp.float32)
    for group in range(N_TP):
        partial_sum = jnp.dot(left[:, group * width:(group + 1) * width], weight[group * width:(group + 1) * width], preferred_element_type=jnp.float32)
        rounded = lax.optimization_barrier(partial_sum.astype(jnp.bfloat16))
        total = total + rounded.astype(jnp.float32)
    return total

def reference(resid, queries, keys, values, decay_pre, out_gate, head_gain, out_proj, mix_gain, mix_shift, gate_in, up_in, down_out, out_gain, out_shift):
    blocks = TOKENS // SPAN
    logdecay = jax.nn.log_sigmoid(decay_pre) / TAU
    scaled_q = queries.astype(jnp.float32).reshape(blocks, SPAN, HEADS, HK) * HK ** (-0.5)
    key_block = keys.astype(jnp.float32).reshape(blocks, SPAN, HEADS, HK)
    value_block = values.astype(jnp.float32).reshape(blocks, SPAN, HEADS, HV)
    cumul = jnp.cumsum(logdecay.reshape(blocks, SPAN, HEADS, HK), axis=1)
    last = cumul[:, -1]
    key_decayed = key_block * jnp.exp(last[:, None] - cumul)

    def advance(running_state, inputs):
        decay_end, current_key, current_value, current_query = inputs
        state_increment = jnp.einsum('tiw,tiz->iwz', current_key, current_value, precision=lax.Precision.HIGHEST)
        running_state = jnp.exp(decay_end)[..., None] * running_state + state_increment
        return (running_state, jnp.einsum('qpy,pyr->qpr', current_query, running_state, precision=lax.Precision.HIGHEST))
    _, state_readout = lax.scan(advance, jnp.zeros((HEADS, HK, HV), jnp.float32), (last, key_decayed, value_block, scaled_q))
    state_readout = state_readout.reshape(TOKENS, HEADS, HV)
    normed = state_readout * lax.rsqrt(lax.optimization_barrier(jnp.mean(state_readout * state_readout, axis=-1, keepdims=True)) + RMS_EPS) * head_gain
    gated = (normed.reshape(TOKENS, VALDIM) * jax.nn.silu(out_gate.astype(jnp.float32))).astype(jnp.bfloat16)
    mixed = group_sum(gated, out_proj, VALDIM // N_TP)
    mid = layer_norm(ALPHA * resid.astype(jnp.float32) + mixed, mix_gain, mix_shift).astype(jnp.bfloat16)

    def channel_mix(middle_block):
        gate = jnp.dot(middle_block, gate_in, preferred_element_type=jnp.float32)
        upward = jnp.dot(middle_block, up_in, preferred_element_type=jnp.float32)
        hidden = (jax.nn.silu(gate) * upward).astype(jnp.bfloat16)
        ffn = group_sum(hidden, down_out, FF // N_TP)
        return layer_norm(ALPHA * middle_block.astype(jnp.float32) + 0.5 * ffn, out_gain, out_shift).astype(jnp.bfloat16)
    result = lax.map(channel_mix, mid.reshape(N_SP, TOK_DEV, D))
    return result.reshape(TOKENS, D)
```

```python
import jax
import jax.numpy as jnp
from jax import lax
from jax.sharding import PartitionSpec as P

HK = 128
HV = 256
SPAN = 64


ALPHA = 2.0**0.25
LN_EPS = 1e-05
RMS_EPS = 1e-06
TAU = 16.0


def entering(array, axis, combine, identity):
    count, place = (lax.axis_size(axis), lax.axis_index(axis))
    everything = jax.tree.map(
        lambda part, kind: lax.all_gather(part.astype(kind), axis),
        array,
        (jnp.bfloat16, jnp.bfloat16),
    )
    start = jax.tree.map(
        lambda part, zero: jnp.broadcast_to(jnp.asarray(zero, part.dtype), part.shape),
        array,
        identity,
    )

    def lap(k, before):
        reached = k < place
        new = combine(
            before, jax.tree.map(lambda part, own: part[k].astype(own.dtype), everything, array)
        )
        return jax.tree.map(lambda a, b: jnp.where(reached, a, b), new, before)

    return lax.fori_loop(0, count, lap, start)


def layer_norm(inputs, gain, shift):
    center = inputs - jnp.mean(inputs, axis=-1, keepdims=True)
    spread = jnp.mean(center * center, axis=-1, keepdims=True)
    return center * lax.rsqrt(spread + LN_EPS) * gain + shift


def combine_states(earlier, later):
    return (earlier[0] * later[0], later[0][..., None] * earlier[1] + later[1])


def incoming_state(own_decay, own_state):
    count = lax.axis_size("sp")
    rows = own_decay.size
    if rows % count:
        identity = (jnp.ones_like(own_decay), jnp.zeros_like(own_state))
        return entering((own_decay, own_state), "sp", combine_states, identity)[1]
    width = own_state.shape[-1]
    decay = own_decay.reshape(count, rows // count, 1)
    high = decay.astype(jnp.bfloat16)
    low = (decay - high.astype(jnp.float32)).astype(jnp.bfloat16)
    sent = jnp.concatenate(
        [own_state.reshape(count, rows // count, width).astype(jnp.bfloat16), high, low], axis=-1
    )
    got = lax.all_to_all(sent, "sp", 0, 0, tiled=True).astype(jnp.float32)
    states, decays = got[..., :width], got[..., width] + got[..., width + 1]
    running = jnp.zeros_like(states[0])
    starts = [running]
    for k in range(count - 1):
        running = decays[k][:, None] * running + states[k]
        starts.append(running)
    back = lax.all_to_all(jnp.stack(starts).astype(jnp.bfloat16), "sp", 0, 0, tiled=True)
    return back.reshape(own_state.shape).astype(jnp.float32)


def mix_tokens(queries, keys, values, decay_pre, out_gate, head_gain):
    tok_rows = queries.shape[0]
    local_heads = queries.shape[1] // HK
    blocks = tok_rows // SPAN
    logdecay = jax.nn.log_sigmoid(decay_pre) / TAU
    scaled_q = queries.astype(jnp.float32).reshape(blocks, SPAN, local_heads, HK) * HK ** (-0.5)
    key_block = keys.astype(jnp.float32).reshape(blocks, SPAN, local_heads, HK)
    value_block = values.astype(jnp.float32).reshape(blocks, SPAN, local_heads, HV)
    cumul = jnp.cumsum(logdecay.reshape(blocks, SPAN, local_heads, HK), axis=1)
    last = cumul[:, -1]
    key_decayed = key_block * jnp.exp(last[:, None] - cumul)
    updates = jnp.einsum(
        "nchk,nchv->nhkv", key_decayed, value_block, precision=lax.Precision.HIGHEST
    )

    def advance(running_state, inputs):
        decay_end, state_increment, current_query = inputs
        running_state = jnp.exp(decay_end)[..., None] * running_state + state_increment
        return (
            running_state,
            jnp.einsum(
                "qpy,pyr->qpr", current_query, running_state, precision=lax.Precision.HIGHEST
            ),
        )

    own_state, local_read = lax.scan(
        advance, jnp.zeros((local_heads, HK, HV), jnp.float32), (last, updates, scaled_q)
    )
    block_ends = jnp.cumsum(last, axis=0)
    own_decay = jnp.exp(block_ends[-1])
    incoming = incoming_state(own_decay, own_state)
    carried = jnp.einsum(
        "xepj,pjw->xepw",
        scaled_q * jnp.exp(block_ends)[:, None],
        incoming,
        precision=lax.Precision.HIGHEST,
    )
    state_readout = (local_read + carried).reshape(tok_rows, local_heads, HV)
    normed = (
        state_readout
        * lax.rsqrt(jnp.mean(state_readout * state_readout, axis=-1, keepdims=True) + RMS_EPS)
        * head_gain
    )
    return (
        normed.reshape(tok_rows, local_heads * HV) * jax.nn.silu(out_gate.astype(jnp.float32))
    ).astype(jnp.bfloat16)


def hidden_by_rows(whole_rows, gate_in, up_in):
    gate = jnp.dot(
        whole_rows,
        lax.all_gather(gate_in, "sp", axis=0, tiled=True),
        preferred_element_type=jnp.float32,
    )
    upward = jnp.dot(
        whole_rows,
        lax.all_gather(up_in, "sp", axis=0, tiled=True),
        preferred_element_type=jnp.float32,
    )
    return (jax.nn.silu(gate) * upward).astype(jnp.bfloat16)


def down_by_columns(hidden, down_out):
    return jnp.dot(
        hidden,
        lax.all_gather(down_out, "sp", axis=1, tiled=True),
        preferred_element_type=jnp.float32,
    )


def own_units(gate_in, up_in, down_out):
    count = lax.axis_size("sp")
    inner, units = gate_in.shape
    piece = units // count
    sent = jnp.concatenate(
        [
            gate_in.T.reshape(count, piece, inner),
            up_in.T.reshape(count, piece, inner),
            down_out.reshape(count, piece, inner),
        ],
        axis=1,
    )
    got = lax.all_to_all(sent, "sp", 0, 0, tiled=True)
    whole = got.transpose(1, 0, 2).reshape(3 * piece, count * inner)
    return whole[:piece], whole[piece : 2 * piece], whole[2 * piece :]


def ffn_by_units(mid, weights):
    gate_t, up_t, down = weights
    rows = lax.all_gather(mid, ("sp", "tp"), axis=0, tiled=True)
    contract = (((1,), (1,)), ((), ()))
    gate = lax.dot_general(rows, gate_t, contract, preferred_element_type=jnp.float32)
    upward = lax.dot_general(rows, up_t, contract, preferred_element_type=jnp.float32)
    hidden = (jax.nn.silu(gate) * upward).astype(jnp.bfloat16)
    part = jnp.dot(hidden, down, preferred_element_type=jnp.float32).astype(jnp.bfloat16)
    return lax.psum_scatter(part, ("sp", "tp"), scatter_dimension=0, tiled=True)


def body(
    resid,
    queries,
    keys,
    values,
    decay_pre,
    out_gate,
    head_gain,
    out_proj,
    mix_gain,
    mix_shift,
    gate_in,
    up_in,
    down_out,
    out_gain,
    out_shift,
):
    tp_count = lax.axis_size("tp")
    tok_rows = queries.shape[0]
    own_count = tok_rows // tp_count
    sp_count = lax.axis_size("sp")
    units = gate_in.shape[1]
    by_units = (
        2 * tok_rows * sp_count < 3 * units
        and units % sp_count == 0
        and (units // sp_count) % 16 == 0
        and gate_in.shape[0] == down_out.shape[1]
    )
    weights = own_units(gate_in, up_in, down_out) if by_units else None
    gated = mix_tokens(queries, keys, values, decay_pre, out_gate, head_gain)
    mixed = lax.psum_scatter(
        jnp.dot(gated, out_proj, preferred_element_type=jnp.float32).astype(jnp.bfloat16),
        "tp",
        scatter_dimension=0,
        tiled=True,
    ).astype(jnp.float32)
    own_resid = lax.dynamic_slice_in_dim(resid, lax.axis_index("tp") * own_count, own_count, 0)
    mid = layer_norm(ALPHA * own_resid.astype(jnp.float32) + mixed, mix_gain, mix_shift).astype(
        jnp.bfloat16
    )
    if by_units:
        ffn = ffn_by_units(mid, weights).astype(jnp.float32)
    else:
        whole_rows = lax.all_gather(mid, "tp", axis=0, tiled=True)
        hidden = hidden_by_rows(whole_rows, gate_in, up_in)
        ffn = lax.psum_scatter(
            down_by_columns(hidden, down_out).astype(jnp.bfloat16),
            "tp",
            scatter_dimension=0,
            tiled=True,
        ).astype(jnp.float32)
    finished = layer_norm(ALPHA * mid.astype(jnp.float32) + 0.5 * ffn, out_gain, out_shift).astype(
        jnp.bfloat16
    )
    return lax.all_gather(finished, "tp", axis=0, tiled=True)


def solution(mesh):
    return jax.shard_map(
        body,
        mesh=mesh,
        in_specs=(
            P("sp", None),
            P("sp", "tp"),
            P("sp", "tp"),
            P("sp", "tp"),
            P("sp", "tp"),
            P("sp", "tp"),
            P(),
            P("tp", None),
            P(),
            P(),
            P("sp", "tp"),
            P("sp", "tp"),
            P("tp", "sp"),
            P(),
            P(),
        ),
        out_specs=P("sp", None),
        check_vma=False,
    )
```

```python
import functools

import jax
import jax.numpy as jnp
from jax import lax
from jax.experimental import pallas as pl
from jax.experimental.pallas import tpu as pltpu
from jax.sharding import PartitionSpec as P

HK = 128
HV = 256
SPAN = 64


ALPHA = 2.0**0.25
LN_EPS = 1e-05
RMS_EPS = 1e-06
TAU = 16.0
MESH = pl.DeviceIdType.MESH


def entering(array, axis, combine, identity):
    count, place = (lax.axis_size(axis), lax.axis_index(axis))
    everything = jax.tree.map(
        lambda part, kind: lax.all_gather(part.astype(kind), axis),
        array,
        (jnp.bfloat16, jnp.bfloat16),
    )
    start = jax.tree.map(
        lambda part, zero: jnp.broadcast_to(jnp.asarray(zero, part.dtype), part.shape),
        array,
        identity,
    )

    def lap(k, before):
        reached = k < place
        new = combine(
            before, jax.tree.map(lambda part, own: part[k].astype(own.dtype), everything, array)
        )
        return jax.tree.map(lambda a, b: jnp.where(reached, a, b), new, before)

    return lax.fori_loop(0, count, lap, start)


def layer_norm(inputs, gain, shift):
    center = inputs - jnp.mean(inputs, axis=-1, keepdims=True)
    spread = jnp.mean(center * center, axis=-1, keepdims=True)
    return center * lax.rsqrt(spread + LN_EPS) * gain + shift


def combine_states(earlier, later):
    return (earlier[0] * later[0], later[0][..., None] * earlier[1] + later[1])


def incoming_state(own_decay, own_state):
    count = lax.axis_size("sp")
    rows = own_decay.size
    if rows % count or (rows // count) % 16:
        identity = (jnp.ones_like(own_decay), jnp.zeros_like(own_state))
        return entering((own_decay, own_state), "sp", combine_states, identity)[1]
    width = own_state.shape[-1]
    decay = own_decay.reshape(count, rows // count, 1)
    high = decay.astype(jnp.bfloat16)
    low = (decay - high.astype(jnp.float32)).astype(jnp.bfloat16)
    fill = jnp.zeros((count, rows // count, 126), jnp.bfloat16)
    sent = jnp.concatenate(
        [own_state.reshape(count, rows // count, width).astype(jnp.bfloat16), high, low, fill],
        axis=-1,
    )
    back = exchange_states(sent, width)
    return back.reshape(own_state.shape).astype(jnp.float32)


def greet(places):
    barrier = pltpu.get_barrier_semaphore()
    for place in places:
        pl.semaphore_signal(barrier, inc=1, device_id=place, device_id_type=MESH)
    pl.semaphore_wait(barrier, len(places))


def remote(src, dst, send, recv, place):
    return pltpu.make_async_remote_copy(
        src_ref=src, dst_ref=dst, send_sem=send, recv_sem=recv, device_id=place, device_id_type=MESH
    )


def states_kernel(count, width, sent, back, got, starts, send1, recv1, send2, recv2, own):
    me, core = lax.axis_index("sp"), lax.axis_index("tp")
    others = [((me + j) % count, core) for j in range(1, count)]
    greet(others)
    first = []
    for j, place in enumerate(others, 1):
        copy = remote(sent.at[place[0]], got.at[me], send1.at[j], recv1.at[j], place)
        copy.start()
        first.append(copy)
    keep = pltpu.make_async_copy(sent.at[me], got.at[me], own.at[0])
    keep.start()
    keep.wait()
    for copy in first:
        copy.wait_recv()
    running = jnp.zeros(starts.shape[1:], jnp.float32)
    for k in range(count):
        starts[k] = running.astype(starts.dtype)
        if k < count - 1:
            piece = got[k].astype(jnp.float32)
            decay = piece[:, width : width + 1] + piece[:, width + 1 : width + 2]
            running = decay * running + piece[:, :width]
    second = []
    for j, place in enumerate(others, 1):
        copy = remote(starts.at[place[0]], back.at[me], send2.at[j], recv2.at[j], place)
        copy.start()
        second.append(copy)
    keep = pltpu.make_async_copy(starts.at[me], back.at[me], own.at[1])
    keep.start()
    keep.wait()
    for copy in second:
        copy.wait_recv()
    for copy in first + second:
        copy.wait_send()


def exchange_states(sent, width):
    count, rows, whole = sent.shape
    return pl.pallas_call(
        functools.partial(states_kernel, count, width),
        out_shape=jax.ShapeDtypeStruct((count, rows, width), sent.dtype),
        in_specs=[pl.BlockSpec(memory_space=pltpu.VMEM)],
        out_specs=pl.BlockSpec(memory_space=pltpu.VMEM),
        scratch_shapes=[
            pltpu.VMEM((count, rows, whole), sent.dtype),
            pltpu.VMEM((count, rows, width), sent.dtype),
            pltpu.SemaphoreType.DMA((count,)),
            pltpu.SemaphoreType.DMA((count,)),
            pltpu.SemaphoreType.DMA((count,)),
            pltpu.SemaphoreType.DMA((count,)),
            pltpu.SemaphoreType.DMA((2,)),
        ],
        compiler_params=pltpu.CompilerParams(collective_id=1, has_side_effects=True),
    )(sent)


def mix_tokens(queries, keys, values, decay_pre, out_gate, head_gain):
    tok_rows = queries.shape[0]
    local_heads = queries.shape[1] // HK
    blocks = tok_rows // SPAN
    logdecay = jax.nn.log_sigmoid(decay_pre) / TAU
    scaled_q = queries.astype(jnp.float32).reshape(blocks, SPAN, local_heads, HK) * HK ** (-0.5)
    key_block = keys.astype(jnp.float32).reshape(blocks, SPAN, local_heads, HK)
    value_block = values.astype(jnp.float32).reshape(blocks, SPAN, local_heads, HV)
    cumul = jnp.cumsum(logdecay.reshape(blocks, SPAN, local_heads, HK), axis=1)
    last = cumul[:, -1]
    key_decayed = key_block * jnp.exp(last[:, None] - cumul)
    updates = jnp.einsum(
        "nchk,nchv->nhkv", key_decayed, value_block, precision=lax.Precision.HIGHEST
    )

    def advance(running_state, inputs):
        decay_end, state_increment, current_query = inputs
        running_state = jnp.exp(decay_end)[..., None] * running_state + state_increment
        return (
            running_state,
            jnp.einsum(
                "qpy,pyr->qpr", current_query, running_state, precision=lax.Precision.HIGHEST
            ),
        )

    own_state, local_read = lax.scan(
        advance, jnp.zeros((local_heads, HK, HV), jnp.float32), (last, updates, scaled_q)
    )
    block_ends = jnp.cumsum(last, axis=0)
    own_decay = jnp.exp(block_ends[-1])
    incoming = incoming_state(own_decay, own_state)
    carried = jnp.einsum(
        "xepj,pjw->xepw",
        scaled_q * jnp.exp(block_ends)[:, None],
        incoming,
        precision=lax.Precision.HIGHEST,
    )
    state_readout = (local_read + carried).reshape(tok_rows, local_heads, HV)
    normed = (
        state_readout
        * lax.rsqrt(jnp.mean(state_readout * state_readout, axis=-1, keepdims=True) + RMS_EPS)
        * head_gain
    )
    return (
        normed.reshape(tok_rows, local_heads * HV) * jax.nn.silu(out_gate.astype(jnp.float32))
    ).astype(jnp.bfloat16)


def hidden_by_rows(whole_rows, gate_in, up_in):
    gate = jnp.dot(
        whole_rows,
        lax.all_gather(gate_in, "sp", axis=0, tiled=True),
        preferred_element_type=jnp.float32,
    )
    upward = jnp.dot(
        whole_rows,
        lax.all_gather(up_in, "sp", axis=0, tiled=True),
        preferred_element_type=jnp.float32,
    )
    return (jax.nn.silu(gate) * upward).astype(jnp.bfloat16)


def down_by_columns(hidden, down_out):
    return jnp.dot(
        hidden,
        lax.all_gather(down_out, "sp", axis=1, tiled=True),
        preferred_element_type=jnp.float32,
    )


def own_units(gate_in, up_in, down_out):
    count = lax.axis_size("sp")
    inner, units = gate_in.shape
    piece = units // count
    sent = jnp.concatenate(
        [
            gate_in.T.reshape(count, piece, inner),
            up_in.T.reshape(count, piece, inner),
            down_out.reshape(count, piece, inner),
        ],
        axis=1,
    )
    return sent


def mixer_kernel(
    count,
    mid,
    sent,
    gain,
    shift,
    out,
    rows,
    weights,
    part,
    twin_in,
    b_out,
    b_in,
    a_out,
    a_in,
    z_out,
    z_in,
    w_send,
    w_recv,
    g_send,
    g_recv,
    t_recv,
    own_sem,
    s_send,
    p_send,
    p_recv,
    b_recv,
    a_recv,
    z_recv,
    f_sem,
):
    me, core = lax.axis_index("sp"), lax.axis_index("tp")
    deep = count // 4
    own, inner = mid.shape
    piece = sent.shape[1] // 3
    lanes = sent.shape[2]
    x, y = me % 2, (me // 2) % 2
    to_x, to_y = 1 - 2 * x, 2 - 4 * y
    to_a = (1 - core) * to_y + core * to_x
    to_b = core * to_y + (1 - core) * to_x
    place_a, place_b = (me + to_a, core), (me + to_b, core)
    twin = (me, 1 - core)
    others = [((me + j) % count, core) for j in range(1, count)]

    def spot(k, a, b):
        return (me + 4 * k) % count + a * to_a + b * to_b

    greet(others + [twin])

    keep = [pltpu.make_async_copy(mid, rows.at[2 * me + core], own_sem.at[0])]
    columns = pl.ds(pl.multiple_of(me * lanes, lanes), lanes)
    keep.append(pltpu.make_async_copy(sent.at[me], weights.at[:, columns], own_sem.at[1]))
    for copy in keep:
        copy.start()

    sends = []

    def forward(k, a, b, place, slot, recv):
        block = 2 * spot(k, a, b) + core
        src = mid if (k, a, b) == (0, 0, 0) else rows.at[block]
        copy = remote(src, rows.at[block], g_send.at[len(sends)], recv.at[slot], place)
        copy.start()
        sends.append(copy)

    def index(k, a, b):
        return (k * 2 + a) * 2 + b

    def landed(k, a, b):
        block = rows.at[2 * spot(k, a, b) + core]
        remote(block, block, g_send.at[0], g_recv.at[index(k, a, b)], twin).wait_recv()

    def onward(k, a, b):
        if not b:
            if not a:
                forward(k, 0, 0, place_a, index(k, 1, 0), g_recv)
            forward(k, a, 0, place_b, index(k, a, 1), g_recv)
        forward(k, a, b, twin, index(k, b, a), t_recv)

    for k in range(1, deep):
        forward(0, 0, 0, ((me + 4 * k) % count, core), index(deep - k, 0, 0), g_recv)
    onward(0, 0, 0)
    moved = []
    for j, place in enumerate(others, 1):
        copy = remote(sent.at[place[0]], weights.at[:, columns], w_send.at[j], w_recv.at[j], place)
        copy.start()
        moved.append(copy)
    order = [(0, 1, 0)] + [(k, 0, 0) for k in range(1, deep)]
    order += [(k, 1, 0) for k in range(1, deep)]
    order += [(k, a, 1) for k in range(deep) for a in range(2)]
    for block in order:
        landed(*block)
        onward(*block)
    for k in range(deep):
        for a in range(2):
            for b in range(2):
                block = rows.at[2 * spot(k, b, a) + 1 - core]
                remote(block, block, g_send.at[0], t_recv.at[index(k, a, b)], twin).wait_recv()
    for copy in keep:
        copy.wait()
    for copy in moved:
        copy.wait_recv()
    for copy in sends + moved:
        copy.wait_send()

    contract = (((1,), (1,)), ((), ()))

    def to_twin(place):
        return remote(
            part.at[2 * place + 1 - core],
            twin_in.at[place],
            p_send.at[place],
            p_recv.at[place],
            twin,
        )

    def tile(i, carry):
        left = rows[pl.ds(4 * i, 4)].reshape(4 * own, inner)
        gate = lax.dot_general(left, weights[:piece], contract, preferred_element_type=jnp.float32)
        up = lax.dot_general(
            left, weights[piece : 2 * piece], contract, preferred_element_type=jnp.float32
        )
        hidden = (gate * jax.nn.sigmoid(gate) * up).astype(jnp.bfloat16)
        down = jnp.dot(hidden, weights[2 * piece :], preferred_element_type=jnp.float32)
        part[pl.ds(4 * i, 4)] = down.astype(jnp.bfloat16).reshape(4, own, inner)
        to_twin(2 * i).start()
        to_twin(2 * i + 1).start()
        return carry

    lax.fori_loop(0, count // 2, tile, 0)

    def summed(k, a, b, arrived):
        place = spot(k, a, b)
        to_twin(place).wait_recv()
        total = part[2 * place + core].astype(jnp.float32) + twin_in[place].astype(jnp.float32)
        for ref, sem, slot in arrived:
            remote(ref.at[slot], ref.at[slot], s_send.at[0], sem.at[slot], twin).wait_recv()
            total = total + ref[slot].astype(jnp.float32)
        return total

    pushed = []

    def push(src, dst, recv, slot, place):
        copy = remote(src.at[slot], dst.at[slot], s_send.at[len(pushed)], recv.at[slot], place)
        copy.start()
        pushed.append(copy)

    turn = [k for k in range(1, deep)] + [0]
    for a in (1, 0):
        for k in turn:
            slot = 2 * k + a
            b_out[slot] = summed(k, a, 1, []).astype(jnp.bfloat16)
            push(b_out, b_in, b_recv, slot, place_b)
    for k in turn:
        a_out[k] = summed(k, 1, 0, [(b_in, b_recv, 2 * k + 1)]).astype(jnp.bfloat16)
        push(a_out, a_in, a_recv, k, place_a)
    for k in range(1, deep):
        z_out[k] = summed(k, 0, 0, [(b_in, b_recv, 2 * k), (a_in, a_recv, k)]).astype(jnp.bfloat16)
        push(z_out, z_in, z_recv, k, ((me + 4 * k) % count, core))
    arrived = [(b_in, b_recv, 0), (a_in, a_recv, 0)] + [(z_in, z_recv, k) for k in range(1, deep)]
    ffn = summed(0, 0, 0, arrived)
    finished = layer_norm(
        ALPHA * mid[...].astype(jnp.float32) + 0.5 * ffn, gain[...], shift[...]
    )
    out[core] = finished.astype(jnp.bfloat16)
    last = remote(out.at[core], out.at[core], f_sem.at[0], f_sem.at[1], twin)
    last.start()

    def drained(place, carry):
        to_twin(place).wait_send()
        return carry

    lax.fori_loop(0, count, drained, 0)
    for copy in pushed:
        copy.wait_send()
    last.wait()


def mixer(mid, sent, gain, shift):
    count = lax.axis_size("sp")
    own, inner = mid.shape
    deep = count // 4
    dma = pltpu.SemaphoreType.DMA
    block = lambda *lead: pltpu.VMEM((*lead, own, inner), jnp.bfloat16)
    out = pl.pallas_call(
        functools.partial(mixer_kernel, count),
        out_shape=jax.ShapeDtypeStruct((2, own, inner), jnp.bfloat16),
        in_specs=[pl.BlockSpec(memory_space=pltpu.VMEM)] * 4,
        out_specs=pl.BlockSpec(memory_space=pltpu.VMEM),
        scratch_shapes=[
            block(2 * count),
            pltpu.VMEM((sent.shape[1], inner), jnp.bfloat16),
            block(2 * count),
            block(count),
            block(2 * deep),
            block(2 * deep),
            block(deep),
            block(deep),
            block(deep),
            block(deep),
            dma((count,)),
            dma((count,)),
            dma((2 * count,)),
            dma((count,)),
            dma((count,)),
            dma((2,)),
            dma((count,)),
            dma((count,)),
            dma((count,)),
            dma((2 * deep,)),
            dma((deep,)),
            dma((deep,)),
            dma((2,)),
        ],
        compiler_params=pltpu.CompilerParams(
            collective_id=2, has_side_effects=True, vmem_limit_bytes=60 * 1024 * 1024
        ),
    )(mid, sent, gain[None], shift[None])
    return out.reshape(2 * own, inner)


def body(
    resid,
    queries,
    keys,
    values,
    decay_pre,
    out_gate,
    head_gain,
    out_proj,
    mix_gain,
    mix_shift,
    gate_in,
    up_in,
    down_out,
    out_gain,
    out_shift,
):
    tp_count = lax.axis_size("tp")
    tok_rows = queries.shape[0]
    own_count = tok_rows // tp_count
    sp_count = lax.axis_size("sp")
    units = gate_in.shape[1]
    by_units = (
        2 * tok_rows * sp_count < 3 * units
        and units % sp_count == 0
        and (units // sp_count) % 16 == 0
        and gate_in.shape[0] == down_out.shape[1]
        and tp_count == 2
        and sp_count % 4 == 0
        and own_count % 16 == 0
    )
    weights = own_units(gate_in, up_in, down_out) if by_units else None
    gated = mix_tokens(queries, keys, values, decay_pre, out_gate, head_gain)
    mixed = lax.psum_scatter(
        jnp.dot(gated, out_proj, preferred_element_type=jnp.float32).astype(jnp.bfloat16),
        "tp",
        scatter_dimension=0,
        tiled=True,
    ).astype(jnp.float32)
    own_resid = lax.dynamic_slice_in_dim(resid, lax.axis_index("tp") * own_count, own_count, 0)
    mid = layer_norm(ALPHA * own_resid.astype(jnp.float32) + mixed, mix_gain, mix_shift).astype(
        jnp.bfloat16
    )
    if by_units:
        return mixer(mid, weights, out_gain, out_shift)
    whole_rows = lax.all_gather(mid, "tp", axis=0, tiled=True)
    hidden = hidden_by_rows(whole_rows, gate_in, up_in)
    ffn = lax.psum_scatter(
        down_by_columns(hidden, down_out).astype(jnp.bfloat16),
        "tp",
        scatter_dimension=0,
        tiled=True,
    ).astype(jnp.float32)
    finished = layer_norm(ALPHA * mid.astype(jnp.float32) + 0.5 * ffn, out_gain, out_shift).astype(
        jnp.bfloat16
    )
    return lax.all_gather(finished, "tp", axis=0, tiled=True)


def solution(mesh):
    return jax.shard_map(
        body,
        mesh=mesh,
        in_specs=(
            P("sp", None),
            P("sp", "tp"),
            P("sp", "tp"),
            P("sp", "tp"),
            P("sp", "tp"),
            P("sp", "tp"),
            P(),
            P("tp", None),
            P(),
            P(),
            P("sp", "tp"),
            P("sp", "tp"),
            P("tp", "sp"),
            P(),
            P(),
        ),
        out_specs=P("sp", None),
        check_vma=False,
    )
```

```python
import functools

import jax
import jax.numpy as jnp
from jax import lax
from jax.experimental import pallas as pl
from jax.experimental.pallas import tpu as pltpu
from jax.sharding import PartitionSpec as P

HK = 128
HV = 256
SPAN = 64


ALPHA = 2.0**0.25
LN_EPS = 1e-05
RMS_EPS = 1e-06
TAU = 16.0
MESH = pl.DeviceIdType.MESH


def entering(array, axis, combine, identity):
    count, place = (lax.axis_size(axis), lax.axis_index(axis))
    everything = jax.tree.map(
        lambda part, kind: lax.all_gather(part.astype(kind), axis),
        array,
        (jnp.bfloat16, jnp.bfloat16),
    )
    start = jax.tree.map(
        lambda part, zero: jnp.broadcast_to(jnp.asarray(zero, part.dtype), part.shape),
        array,
        identity,
    )

    def lap(k, before):
        reached = k < place
        new = combine(
            before, jax.tree.map(lambda part, own: part[k].astype(own.dtype), everything, array)
        )
        return jax.tree.map(lambda a, b: jnp.where(reached, a, b), new, before)

    return lax.fori_loop(0, count, lap, start)


def layer_norm(inputs, gain, shift):
    center = inputs - jnp.mean(inputs, axis=-1, keepdims=True)
    spread = jnp.mean(center * center, axis=-1, keepdims=True)
    return center * lax.rsqrt(spread + LN_EPS) * gain + shift


def combine_states(earlier, later):
    return (earlier[0] * later[0], later[0][..., None] * earlier[1] + later[1])


def packed_state(own_decay, own_state):
    count = lax.axis_size("sp")
    rows, width = own_decay.size, own_state.shape[-1]
    decay = own_decay.reshape(count, rows // count, 1)
    high = decay.astype(jnp.bfloat16)
    low = (decay - high.astype(jnp.float32)).astype(jnp.bfloat16)
    fill = jnp.zeros((count, rows // count, 126), jnp.bfloat16)
    return jnp.concatenate(
        [own_state.reshape(count, rows // count, width).astype(jnp.bfloat16), high, low, fill],
        axis=-1,
    )


def greet(places):
    barrier = pltpu.get_barrier_semaphore()
    for place in places:
        pl.semaphore_signal(barrier, inc=1, device_id=place, device_id_type=MESH)
    pl.semaphore_wait(barrier, len(places))


def remote(src, dst, send, recv, place):
    return pltpu.make_async_remote_copy(
        src_ref=src, dst_ref=dst, send_sem=send, recv_sem=recv, device_id=place, device_id_type=MESH
    )


def local_tokens(queries, keys, values, decay_pre):
    tok_rows = queries.shape[0]
    local_heads = queries.shape[1] // HK
    blocks = tok_rows // SPAN
    logdecay = jax.nn.log_sigmoid(decay_pre) / TAU
    scaled_q = queries.astype(jnp.float32).reshape(blocks, SPAN, local_heads, HK) * HK ** (-0.5)
    key_block = keys.astype(jnp.float32).reshape(blocks, SPAN, local_heads, HK)
    value_block = values.astype(jnp.float32).reshape(blocks, SPAN, local_heads, HV)
    cumul = jnp.cumsum(logdecay.reshape(blocks, SPAN, local_heads, HK), axis=1)
    last = cumul[:, -1]
    key_decayed = key_block * jnp.exp(last[:, None] - cumul)
    updates = jnp.einsum(
        "nchk,nchv->nhkv", key_decayed, value_block, precision=lax.Precision.HIGHEST
    )

    def advance(running_state, inputs):
        decay_end, state_increment, current_query = inputs
        running_state = jnp.exp(decay_end)[..., None] * running_state + state_increment
        return (
            running_state,
            jnp.einsum(
                "qpy,pyr->qpr", current_query, running_state, precision=lax.Precision.HIGHEST
            ),
        )

    own_state, local_read = lax.scan(
        advance, jnp.zeros((local_heads, HK, HV), jnp.float32), (last, updates, scaled_q)
    )
    block_ends = jnp.cumsum(last, axis=0)
    own_decay = jnp.exp(block_ends[-1])
    carry_q = scaled_q * jnp.exp(block_ends)[:, None]
    return local_read, carry_q, own_decay, own_state


def mix_tokens(local_read, carry_q, own_decay, own_state, out_gate, head_gain):
    blocks, span, local_heads, _ = carry_q.shape
    tok_rows = blocks * span
    identity = (jnp.ones_like(own_decay), jnp.zeros_like(own_state))
    _, incoming = entering((own_decay, own_state), "sp", combine_states, identity)
    carried = jnp.einsum(
        "xepj,pjw->xepw", carry_q, incoming, precision=lax.Precision.HIGHEST
    )
    state_readout = (local_read + carried).reshape(tok_rows, local_heads, HV)
    normed = (
        state_readout
        * lax.rsqrt(jnp.mean(state_readout * state_readout, axis=-1, keepdims=True) + RMS_EPS)
        * head_gain
    )
    return (
        normed.reshape(tok_rows, local_heads * HV) * jax.nn.silu(out_gate.astype(jnp.float32))
    ).astype(jnp.bfloat16)


def hidden_by_rows(whole_rows, gate_in, up_in):
    gate = jnp.dot(
        whole_rows,
        lax.all_gather(gate_in, "sp", axis=0, tiled=True),
        preferred_element_type=jnp.float32,
    )
    upward = jnp.dot(
        whole_rows,
        lax.all_gather(up_in, "sp", axis=0, tiled=True),
        preferred_element_type=jnp.float32,
    )
    return (jax.nn.silu(gate) * upward).astype(jnp.bfloat16)


def down_by_columns(hidden, down_out):
    return jnp.dot(
        hidden,
        lax.all_gather(down_out, "sp", axis=1, tiled=True),
        preferred_element_type=jnp.float32,
    )


def own_units(gate_in, up_in, down_out):
    count = lax.axis_size("sp")
    inner, units = gate_in.shape
    piece = units // count
    sent = jnp.concatenate(
        [
            gate_in.T.reshape(count, piece, inner),
            up_in.T.reshape(count, piece, inner),
            down_out.reshape(count, piece, inner),
        ],
        axis=1,
    )
    return sent


def layer_kernel(
    count,
    width,
    states,
    local_read,
    carry_q,
    out_gate,
    head_gain,
    out_proj,
    resid,
    mix_gain,
    mix_shift,
    sent,
    gain,
    shift,
    out,
    got,
    starts,
    back,
    proj,
    gated,
    mixed,
    mixed_in,
    mid,
    rows,
    weights,
    part,
    twin_in,
    b_out,
    b_in,
    a_out,
    a_in,
    z_out,
    z_in,
    send1,
    recv1,
    send2,
    recv2,
    m_sem,
    w_send,
    w_recv,
    g_send,
    g_recv,
    t_recv,
    own_sem,
    s_send,
    p_send,
    p_recv,
    b_recv,
    a_recv,
    z_recv,
    f_sem,
):
    me, core = lax.axis_index("sp"), lax.axis_index("tp")
    deep = count // 4
    own, inner = mid.shape
    piece = sent.shape[1] // 3
    lanes = sent.shape[2]
    x, y = me % 2, (me // 2) % 2
    to_x, to_y = 1 - 2 * x, 2 - 4 * y
    to_a = (1 - core) * to_y + core * to_x
    to_b = core * to_y + (1 - core) * to_x
    place_a, place_b = (me + to_a, core), (me + to_b, core)
    twin = (me, 1 - core)
    others = [((me + j) % count, core) for j in range(1, count)]

    def spot(k, a, b):
        return (me + 4 * k) % count + a * to_a + b * to_b

    greet(others + [twin])

    moved = []
    for j, place in enumerate(others, 1):
        copy = remote(states.at[place[0]], got.at[me], send1.at[j], recv1.at[j], place)
        copy.start()
        moved.append(copy)
    columns = pl.ds(pl.multiple_of(me * lanes, lanes), lanes)
    keep = [
        pltpu.make_async_copy(states.at[me], got.at[me], own_sem.at[0]),
        pltpu.make_async_copy(out_proj, proj, own_sem.at[1]),
        pltpu.make_async_copy(sent.at[me], weights.at[:, columns], own_sem.at[2]),
    ]
    for copy in keep:
        copy.start()
    keep[0].wait()
    for copy in moved:
        copy.wait_recv()
    running = jnp.zeros(starts.shape[1:], jnp.float32)
    for k in range(count):
        starts[k] = running.astype(starts.dtype)
        if k < count - 1:
            state = got[k].astype(jnp.float32)
            decay = state[:, width : width + 1] + state[:, width + 1 : width + 2]
            running = decay * running + state[:, :width]
    returned = []
    for j, place in enumerate(others, 1):
        copy = remote(starts.at[place[0]], back.at[me], send2.at[j], recv2.at[j], place)
        copy.start()
        returned.append(copy)
    mine = pltpu.make_async_copy(starts.at[me], back.at[me], own_sem.at[3])
    mine.start()
    brought = []
    for j, place in enumerate(others, 1):
        copy = remote(sent.at[place[0]], weights.at[:, columns], w_send.at[j], w_recv.at[j], place)
        copy.start()
        brought.append(copy)
    mine.wait()
    for copy in returned:
        copy.wait_recv()

    heads = gated.shape[1] // width
    key_width = carry_q.shape[1] // heads
    each = count // heads
    for h in range(heads):
        wide = slice(h * width, (h + 1) * width)
        incoming = back[h * each : (h + 1) * each].reshape(key_width, width).astype(jnp.float32)
        read = local_read[:, wide] + jnp.dot(
            carry_q[:, h * key_width : (h + 1) * key_width],
            incoming,
            precision=lax.Precision.HIGHEST,
            preferred_element_type=jnp.float32,
        )
        size = jnp.mean(read * read, axis=-1, keepdims=True)
        pre = out_gate[:, wide].astype(jnp.float32)
        normed = read * lax.rsqrt(size + RMS_EPS) * head_gain[...]
        gated[:, wide] = (normed * (pre * jax.nn.sigmoid(pre))).astype(jnp.bfloat16)
    keep[1].wait()
    summed_heads = jnp.dot(gated[...], proj[...], preferred_element_type=jnp.float32)
    mixed[...] = summed_heads.astype(jnp.bfloat16).reshape(2, own, inner)
    swap = remote(mixed.at[1 - core], mixed_in, m_sem.at[0], m_sem.at[1], twin)
    swap.start()
    swap.wait()
    total = mixed[core].astype(jnp.float32) + mixed_in[...].astype(jnp.float32)
    before = ALPHA * resid[core].astype(jnp.float32) + total
    middle = layer_norm(before, mix_gain[...], mix_shift[...]).astype(jnp.bfloat16)
    mid[...] = middle
    rows[2 * me + core] = middle

    sends = []

    def forward(k, a, b, place, slot, recv):
        block = 2 * spot(k, a, b) + core
        src = mid if (k, a, b) == (0, 0, 0) else rows.at[block]
        copy = remote(src, rows.at[block], g_send.at[len(sends)], recv.at[slot], place)
        copy.start()
        sends.append(copy)

    def index(k, a, b):
        return (k * 2 + a) * 2 + b

    def landed(k, a, b):
        block = rows.at[2 * spot(k, a, b) + core]
        remote(block, block, g_send.at[0], g_recv.at[index(k, a, b)], twin).wait_recv()

    def onward(k, a, b):
        if not b:
            if not a:
                forward(k, 0, 0, place_a, index(k, 1, 0), g_recv)
            forward(k, a, 0, place_b, index(k, a, 1), g_recv)
        forward(k, a, b, twin, index(k, b, a), t_recv)

    for k in range(1, deep):
        forward(0, 0, 0, ((me + 4 * k) % count, core), index(deep - k, 0, 0), g_recv)
    onward(0, 0, 0)
    order = [(0, 1, 0)] + [(k, 0, 0) for k in range(1, deep)]
    order += [(k, 1, 0) for k in range(1, deep)]
    order += [(k, a, 1) for k in range(deep) for a in range(2)]
    for block in order:
        landed(*block)
        onward(*block)
    for k in range(deep):
        for a in range(2):
            for b in range(2):
                block = rows.at[2 * spot(k, b, a) + 1 - core]
                remote(block, block, g_send.at[0], t_recv.at[index(k, a, b)], twin).wait_recv()
    keep[2].wait()
    for copy in brought:
        copy.wait_recv()
    for copy in sends + moved + returned + brought:
        copy.wait_send()

    contract = (((1,), (1,)), ((), ()))

    def to_twin(place):
        return remote(
            part.at[2 * place + 1 - core],
            twin_in.at[place],
            p_send.at[place],
            p_recv.at[place],
            twin,
        )

    def tile(step, side):
        i = 2 * ((me // 4 + step) % deep) + side
        left = rows[pl.ds(4 * i, 4)].reshape(4 * own, inner)
        gate = lax.dot_general(left, weights[:piece], contract, preferred_element_type=jnp.float32)
        up = lax.dot_general(
            left, weights[piece : 2 * piece], contract, preferred_element_type=jnp.float32
        )
        hidden = (gate * jax.nn.sigmoid(gate) * up).astype(jnp.bfloat16)
        down = jnp.dot(hidden, weights[2 * piece :], preferred_element_type=jnp.float32)
        part[pl.ds(4 * i, 4)] = down.astype(jnp.bfloat16).reshape(4, own, inner)
        to_twin(2 * i).start()
        to_twin(2 * i + 1).start()
        return side

    def summed(k, a, b, arrived):
        place = spot(k, a, b)
        to_twin(place).wait_recv()
        total = part[2 * place + core].astype(jnp.float32) + twin_in[place].astype(jnp.float32)
        for ref, sem, slot in arrived:
            remote(ref.at[slot], ref.at[slot], s_send.at[0], sem.at[slot], twin).wait_recv()
            total = total + ref[slot].astype(jnp.float32)
        return total

    pushed = []

    def push(src, dst, recv, slot, place):
        copy = remote(src.at[slot], dst.at[slot], s_send.at[len(pushed)], recv.at[slot], place)
        copy.start()
        pushed.append(copy)

    turn = [k for k in range(1, deep)] + [0]
    for a in (1, 0):
        lax.fori_loop(0, deep, tile, a * (1 - y) + (1 - a) * y)
        for k in turn:
            slot = 2 * k + a
            b_out[slot] = summed(k, a, 1, []).astype(jnp.bfloat16)
            push(b_out, b_in, b_recv, slot, place_b)
    for k in turn:
        a_out[k] = summed(k, 1, 0, [(b_in, b_recv, 2 * k + 1)]).astype(jnp.bfloat16)
        push(a_out, a_in, a_recv, k, place_a)
    for k in range(1, deep):
        z_out[k] = summed(k, 0, 0, [(b_in, b_recv, 2 * k), (a_in, a_recv, k)]).astype(jnp.bfloat16)
        push(z_out, z_in, z_recv, k, ((me + 4 * k) % count, core))
    arrived = [(b_in, b_recv, 0), (a_in, a_recv, 0)] + [(z_in, z_recv, k) for k in range(1, deep)]
    ffn = summed(0, 0, 0, arrived)
    finished = layer_norm(
        ALPHA * mid[...].astype(jnp.float32) + 0.5 * ffn, gain[...], shift[...]
    )
    out[core] = finished.astype(jnp.bfloat16)
    last = remote(out.at[core], out.at[core], f_sem.at[0], f_sem.at[1], twin)
    last.start()

    def drained(place, carry):
        to_twin(place).wait_send()
        return carry

    lax.fori_loop(0, count, drained, 0)
    for copy in pushed:
        copy.wait_send()
    last.wait()


def layer(local, out_gate, head_gain, out_proj, resid, mix_gain, mix_shift, sent, gain, shift):
    local_read, carry_q, own_decay, own_state = local
    count = lax.axis_size("sp")
    tok_rows, inner = resid.shape
    own = tok_rows // 2
    deep = count // 4
    states = packed_state(own_decay, own_state)
    _, slice_rows, wide = states.shape
    width = own_state.shape[-1]
    dma = pltpu.SemaphoreType.DMA
    block = lambda *lead: pltpu.VMEM((*lead, own, inner), jnp.bfloat16)
    near, far = pl.BlockSpec(memory_space=pltpu.VMEM), pl.BlockSpec(memory_space=pl.ANY)
    out = pl.pallas_call(
        functools.partial(layer_kernel, count, width),
        out_shape=jax.ShapeDtypeStruct((2, own, inner), jnp.bfloat16),
        in_specs=[near] * 5 + [far] + [near] * 3 + [far] + [near] * 2,
        out_specs=near,
        scratch_shapes=[
            pltpu.VMEM((count, slice_rows, wide), jnp.bfloat16),
            pltpu.VMEM((count, slice_rows, width), jnp.bfloat16),
            pltpu.VMEM((count, slice_rows, width), jnp.bfloat16),
            pltpu.VMEM(out_proj.shape, jnp.bfloat16),
            pltpu.VMEM((tok_rows, out_proj.shape[0]), jnp.bfloat16),
            block(2),
            block(),
            block(),
            block(2 * count),
            pltpu.VMEM((sent.shape[1], inner), jnp.bfloat16),
            block(2 * count),
            block(count),
            block(2 * deep),
            block(2 * deep),
            block(deep),
            block(deep),
            block(deep),
            block(deep),
            dma((count,)),
            dma((count,)),
            dma((count,)),
            dma((count,)),
            dma((2,)),
            dma((count,)),
            dma((count,)),
            dma((2 * count,)),
            dma((count,)),
            dma((count,)),
            dma((4,)),
            dma((count,)),
            dma((count,)),
            dma((count,)),
            dma((2 * deep,)),
            dma((deep,)),
            dma((deep,)),
            dma((2,)),
        ],
        compiler_params=pltpu.CompilerParams(
            collective_id=2, has_side_effects=True, vmem_limit_bytes=60 * 1024 * 1024
        ),
    )(
        states,
        local_read.reshape(tok_rows, -1),
        carry_q.reshape(tok_rows, -1),
        out_gate,
        head_gain[None],
        out_proj,
        resid.reshape(2, own, inner),
        mix_gain[None],
        mix_shift[None],
        sent,
        gain[None],
        shift[None],
    )
    return out.reshape(tok_rows, inner)


def body(
    resid,
    queries,
    keys,
    values,
    decay_pre,
    out_gate,
    head_gain,
    out_proj,
    mix_gain,
    mix_shift,
    gate_in,
    up_in,
    down_out,
    out_gain,
    out_shift,
):
    tp_count = lax.axis_size("tp")
    tok_rows = queries.shape[0]
    own_count = tok_rows // tp_count
    sp_count = lax.axis_size("sp")
    units = gate_in.shape[1]
    key_rows, heads = queries.shape[1], queries.shape[1] // HK
    by_units = (
        2 * tok_rows * sp_count < 3 * units
        and units % sp_count == 0
        and (units // sp_count) % 16 == 0
        and gate_in.shape[0] == down_out.shape[1]
        and tp_count == 2
        and sp_count % 4 == 0
        and own_count % 16 == 0
        and key_rows % (16 * sp_count) == 0
        and sp_count % heads == 0
    )
    local = local_tokens(queries, keys, values, decay_pre)
    if by_units:
        sent = own_units(gate_in, up_in, down_out)
        norms = (mix_gain, mix_shift, sent, out_gain, out_shift)
        return layer(local, out_gate, head_gain, out_proj, resid, *norms)
    gated = mix_tokens(*local, out_gate, head_gain)
    mixed = lax.psum_scatter(
        jnp.dot(gated, out_proj, preferred_element_type=jnp.float32).astype(jnp.bfloat16),
        "tp",
        scatter_dimension=0,
        tiled=True,
    ).astype(jnp.float32)
    own_resid = lax.dynamic_slice_in_dim(resid, lax.axis_index("tp") * own_count, own_count, 0)
    mid = layer_norm(ALPHA * own_resid.astype(jnp.float32) + mixed, mix_gain, mix_shift).astype(
        jnp.bfloat16
    )
    whole_rows = lax.all_gather(mid, "tp", axis=0, tiled=True)
    hidden = hidden_by_rows(whole_rows, gate_in, up_in)
    ffn = lax.psum_scatter(
        down_by_columns(hidden, down_out).astype(jnp.bfloat16),
        "tp",
        scatter_dimension=0,
        tiled=True,
    ).astype(jnp.float32)
    finished = layer_norm(ALPHA * mid.astype(jnp.float32) + 0.5 * ffn, out_gain, out_shift).astype(
        jnp.bfloat16
    )
    return lax.all_gather(finished, "tp", axis=0, tiled=True)


def solution(mesh):
    return jax.shard_map(
        body,
        mesh=mesh,
        in_specs=(
            P("sp", None),
            P("sp", "tp"),
            P("sp", "tp"),
            P("sp", "tp"),
            P("sp", "tp"),
            P("sp", "tp"),
            P(),
            P("tp", None),
            P(),
            P(),
            P("sp", "tp"),
            P("sp", "tp"),
            P("tp", "sp"),
            P(),
            P(),
        ),
        out_specs=P("sp", None),
        check_vma=False,
    )
```

```python
import functools

import jax
import jax.numpy as jnp
from jax import lax
from jax.experimental import pallas as pl
from jax.experimental.pallas import tpu as pltpu
from jax.sharding import PartitionSpec as P

HK = 128
HV = 256
SPAN = 64


ALPHA = 2.0**0.25
LN_EPS = 1e-05
RMS_EPS = 1e-06
TAU = 16.0
MESH = pl.DeviceIdType.MESH


def entering(array, axis, combine, identity):
    count, place = (lax.axis_size(axis), lax.axis_index(axis))
    everything = jax.tree.map(
        lambda part, kind: lax.all_gather(part.astype(kind), axis),
        array,
        (jnp.bfloat16, jnp.bfloat16),
    )
    start = jax.tree.map(
        lambda part, zero: jnp.broadcast_to(jnp.asarray(zero, part.dtype), part.shape),
        array,
        identity,
    )

    def lap(k, before):
        reached = k < place
        new = combine(
            before, jax.tree.map(lambda part, own: part[k].astype(own.dtype), everything, array)
        )
        return jax.tree.map(lambda a, b: jnp.where(reached, a, b), new, before)

    return lax.fori_loop(0, count, lap, start)


def layer_norm(inputs, gain, shift):
    center = inputs - jnp.mean(inputs, axis=-1, keepdims=True)
    spread = jnp.mean(center * center, axis=-1, keepdims=True)
    return center * lax.rsqrt(spread + LN_EPS) * gain + shift


def combine_states(earlier, later):
    return (earlier[0] * later[0], later[0][..., None] * earlier[1] + later[1])


def packed_state(own_decay, own_state):
    count = lax.axis_size("sp")
    rows, width = own_decay.size, own_state.shape[-1]
    decay = own_decay.reshape(count, rows // count, 1)
    high = decay.astype(jnp.bfloat16)
    low = (decay - high.astype(jnp.float32)).astype(jnp.bfloat16)
    fill = jnp.zeros((count, rows // count, 126), jnp.bfloat16)
    return jnp.concatenate(
        [own_state.reshape(count, rows // count, width).astype(jnp.bfloat16), high, low, fill],
        axis=-1,
    )


def greet(places):
    barrier = pltpu.get_barrier_semaphore()
    for place in places:
        pl.semaphore_signal(barrier, inc=1, device_id=place, device_id_type=MESH)
    pl.semaphore_wait(barrier, len(places))


def remote(src, dst, send, recv, place):
    return pltpu.make_async_remote_copy(
        src_ref=src, dst_ref=dst, send_sem=send, recv_sem=recv, device_id=place, device_id_type=MESH
    )


def local_tokens(queries, keys, values, decay_pre):
    tok_rows = queries.shape[0]
    local_heads = queries.shape[1] // HK
    blocks = tok_rows // SPAN
    logdecay = jax.nn.log_sigmoid(decay_pre) / TAU
    scaled_q = queries.astype(jnp.float32).reshape(blocks, SPAN, local_heads, HK) * HK ** (-0.5)
    key_block = keys.astype(jnp.float32).reshape(blocks, SPAN, local_heads, HK)
    value_block = values.astype(jnp.float32).reshape(blocks, SPAN, local_heads, HV)
    cumul = jnp.cumsum(logdecay.reshape(blocks, SPAN, local_heads, HK), axis=1)
    last = cumul[:, -1]
    key_decayed = key_block * jnp.exp(last[:, None] - cumul)
    updates = jnp.einsum(
        "nchk,nchv->nhkv", key_decayed, value_block, precision=lax.Precision.HIGHEST
    )

    def advance(running_state, inputs):
        decay_end, state_increment, current_query = inputs
        running_state = jnp.exp(decay_end)[..., None] * running_state + state_increment
        return (
            running_state,
            jnp.einsum(
                "qpy,pyr->qpr", current_query, running_state, precision=lax.Precision.HIGHEST
            ),
        )

    own_state, local_read = lax.scan(
        advance, jnp.zeros((local_heads, HK, HV), jnp.float32), (last, updates, scaled_q)
    )
    block_ends = jnp.cumsum(last, axis=0)
    own_decay = jnp.exp(block_ends[-1])
    carry_q = scaled_q * jnp.exp(block_ends)[:, None]
    return local_read, carry_q, own_decay, own_state


def mix_tokens(local_read, carry_q, own_decay, own_state, out_gate, head_gain):
    blocks, span, local_heads, _ = carry_q.shape
    tok_rows = blocks * span
    identity = (jnp.ones_like(own_decay), jnp.zeros_like(own_state))
    _, incoming = entering((own_decay, own_state), "sp", combine_states, identity)
    carried = jnp.einsum(
        "xepj,pjw->xepw", carry_q, incoming, precision=lax.Precision.HIGHEST
    )
    state_readout = (local_read + carried).reshape(tok_rows, local_heads, HV)
    normed = (
        state_readout
        * lax.rsqrt(jnp.mean(state_readout * state_readout, axis=-1, keepdims=True) + RMS_EPS)
        * head_gain
    )
    return (
        normed.reshape(tok_rows, local_heads * HV) * jax.nn.silu(out_gate.astype(jnp.float32))
    ).astype(jnp.bfloat16)


def hidden_by_rows(whole_rows, gate_in, up_in):
    gate = jnp.dot(
        whole_rows,
        lax.all_gather(gate_in, "sp", axis=0, tiled=True),
        preferred_element_type=jnp.float32,
    )
    upward = jnp.dot(
        whole_rows,
        lax.all_gather(up_in, "sp", axis=0, tiled=True),
        preferred_element_type=jnp.float32,
    )
    return (jax.nn.silu(gate) * upward).astype(jnp.bfloat16)


def down_by_columns(hidden, down_out):
    return jnp.dot(
        hidden,
        lax.all_gather(down_out, "sp", axis=1, tiled=True),
        preferred_element_type=jnp.float32,
    )


def own_units(gate_in, up_in, down_out):
    count = lax.axis_size("sp")
    inner, units = gate_in.shape
    piece = units // count
    sent = jnp.concatenate(
        [
            gate_in.T.reshape(count, piece, inner),
            up_in.T.reshape(count, piece, inner),
            down_out.reshape(count, piece, inner),
        ],
        axis=1,
    )
    return sent


def layer_kernel(
    count,
    width,
    states,
    local_read,
    carry_q,
    out_gate,
    head_gain,
    out_proj,
    resid,
    mix_gain,
    mix_shift,
    sent,
    gain,
    shift,
    out,
    got,
    starts,
    back,
    proj,
    gated,
    mixed,
    mixed_in,
    mid,
    rows,
    weights,
    part,
    twin_in,
    b_out,
    b_in,
    a_out,
    a_in,
    z_out,
    z_in,
    send1,
    recv1,
    send2,
    recv2,
    m_sem,
    w_send,
    w_recv,
    g_send,
    g_recv,
    t_recv,
    own_sem,
    s_send,
    p_send,
    p_recv,
    b_recv,
    a_recv,
    z_recv,
    f_sem,
):
    me, core = lax.axis_index("sp"), lax.axis_index("tp")
    deep = count // 4
    own, inner = mid.shape
    piece = sent.shape[1] // 3
    lanes = sent.shape[2]
    x, y = me % 2, (me // 2) % 2
    to_x, to_y = 1 - 2 * x, 2 - 4 * y
    to_a = (1 - core) * to_y + core * to_x
    to_b = core * to_y + (1 - core) * to_x
    place_a, place_b = (me + to_a, core), (me + to_b, core)
    twin = (me, 1 - core)
    others = [((me + j) % count, core) for j in range(1, count)]

    def spot(k, a, b):
        return (me + 4 * k) % count + a * to_a + b * to_b

    greet(others + [twin])

    moved = []
    for j, place in enumerate(others, 1):
        copy = remote(states.at[place[0]], got.at[me], send1.at[j], recv1.at[j], place)
        copy.start()
        moved.append(copy)
    columns = pl.ds(pl.multiple_of(me * lanes, lanes), lanes)
    keep = [
        pltpu.make_async_copy(states.at[me], got.at[me], own_sem.at[0]),
        pltpu.make_async_copy(out_proj, proj, own_sem.at[1]),
        pltpu.make_async_copy(sent.at[me], weights.at[:, columns], own_sem.at[2]),
    ]
    for copy in keep:
        copy.start()
    keep[0].wait()
    for copy in moved:
        copy.wait_recv()
    running = jnp.zeros(starts.shape[1:], jnp.float32)
    for k in range(count):
        starts[k] = running.astype(starts.dtype)
        if k < count - 1:
            state = got[k].astype(jnp.float32)
            decay = state[:, width : width + 1] + state[:, width + 1 : width + 2]
            running = decay * running + state[:, :width]
    returned = []
    for j, place in enumerate(others, 1):
        copy = remote(starts.at[place[0]], back.at[me], send2.at[j], recv2.at[j], place)
        copy.start()
        returned.append(copy)
    mine = pltpu.make_async_copy(starts.at[me], back.at[me], own_sem.at[3])
    mine.start()
    brought = []

    def bring(first, last):
        taken = pl.ds(first * piece, (last - first) * piece)
        for place in others:
            slot = len(brought)
            copy = remote(
                sent.at[place[0], taken],
                weights.at[taken, columns],
                w_send.at[slot],
                w_recv.at[slot],
                place,
            )
            copy.start()
            brought.append(copy)

    bring(0, 1)
    mine.wait()
    for copy in returned:
        copy.wait_recv()

    heads = gated.shape[1] // width
    key_width = carry_q.shape[1] // heads
    each = count // heads
    for h in range(heads):
        wide = slice(h * width, (h + 1) * width)
        incoming = back[h * each : (h + 1) * each].reshape(key_width, width).astype(jnp.float32)
        read = local_read[:, wide] + jnp.dot(
            carry_q[:, h * key_width : (h + 1) * key_width],
            incoming,
            precision=lax.Precision.HIGHEST,
            preferred_element_type=jnp.float32,
        )
        size = jnp.mean(read * read, axis=-1, keepdims=True)
        pre = out_gate[:, wide].astype(jnp.float32)
        normed = read * lax.rsqrt(size + RMS_EPS) * head_gain[...]
        gated[:, wide] = (normed * (pre * jax.nn.sigmoid(pre))).astype(jnp.bfloat16)
    keep[1].wait()
    summed_heads = jnp.dot(gated[...], proj[...], preferred_element_type=jnp.float32)
    mixed[...] = summed_heads.astype(jnp.bfloat16).reshape(2, own, inner)
    swap = remote(mixed.at[1 - core], mixed_in, m_sem.at[0], m_sem.at[1], twin)
    swap.start()
    swap.wait()
    total = mixed[core].astype(jnp.float32) + mixed_in[...].astype(jnp.float32)
    before = ALPHA * resid[core].astype(jnp.float32) + total
    middle = layer_norm(before, mix_gain[...], mix_shift[...]).astype(jnp.bfloat16)
    mid[...] = middle
    rows[2 * me + core] = middle

    sends = []

    def forward(k, a, b, place, slot, recv):
        block = 2 * spot(k, a, b) + core
        src = mid if (k, a, b) == (0, 0, 0) else rows.at[block]
        copy = remote(src, rows.at[block], g_send.at[len(sends)], recv.at[slot], place)
        copy.start()
        sends.append(copy)

    def index(k, a, b):
        return (k * 2 + a) * 2 + b

    def landed(k, a, b):
        block = rows.at[2 * spot(k, a, b) + core]
        remote(block, block, g_send.at[0], g_recv.at[index(k, a, b)], twin).wait_recv()

    def onward(k, a, b):
        if not b:
            if not a:
                forward(k, 0, 0, place_a, index(k, 1, 0), g_recv)
            forward(k, a, 0, place_b, index(k, a, 1), g_recv)
        forward(k, a, b, twin, index(k, b, a), t_recv)

    for k in range(1, deep):
        forward(0, 0, 0, ((me + 4 * k) % count, core), index(deep - k, 0, 0), g_recv)
    onward(0, 0, 0)
    bring(1, 3)
    order = [(0, 1, 0)] + [(k, 0, 0) for k in range(1, deep)]
    order += [(k, 1, 0) for k in range(1, deep)]
    order += [(k, a, 1) for k in range(deep) for a in range(2)]
    for block in order:
        landed(*block)
        onward(*block)
    for k in range(deep):
        for a in range(2):
            for b in range(2):
                block = rows.at[2 * spot(k, b, a) + 1 - core]
                remote(block, block, g_send.at[0], t_recv.at[index(k, a, b)], twin).wait_recv()
    keep[2].wait()
    for copy in brought:
        copy.wait_recv()
    for copy in sends + moved + returned + brought:
        copy.wait_send()

    contract = (((1,), (1,)), ((), ()))

    def to_twin(place):
        return remote(
            part.at[2 * place + 1 - core],
            twin_in.at[place],
            p_send.at[place],
            p_recv.at[place],
            twin,
        )

    def tile(step, side):
        i = 2 * ((me // 4 + step) % deep) + side
        left = rows[pl.ds(4 * i, 4)].reshape(4 * own, inner)
        gate = lax.dot_general(left, weights[:piece], contract, preferred_element_type=jnp.float32)
        up = lax.dot_general(
            left, weights[piece : 2 * piece], contract, preferred_element_type=jnp.float32
        )
        hidden = (gate * jax.nn.sigmoid(gate) * up).astype(jnp.bfloat16)
        down = jnp.dot(hidden, weights[2 * piece :], preferred_element_type=jnp.float32)
        part[pl.ds(4 * i, 4)] = down.astype(jnp.bfloat16).reshape(4, own, inner)
        to_twin(2 * i).start()
        to_twin(2 * i + 1).start()
        return side

    def summed(k, a, b, arrived):
        place = spot(k, a, b)
        to_twin(place).wait_recv()
        total = part[2 * place + core].astype(jnp.float32) + twin_in[place].astype(jnp.float32)
        for ref, sem, slot in arrived:
            remote(ref.at[slot], ref.at[slot], s_send.at[0], sem.at[slot], twin).wait_recv()
            total = total + ref[slot].astype(jnp.float32)
        return total

    pushed = []

    def push(src, dst, recv, slot, place):
        copy = remote(src.at[slot], dst.at[slot], s_send.at[len(pushed)], recv.at[slot], place)
        copy.start()
        pushed.append(copy)

    turn = [k for k in range(1, deep)] + [0]
    for a in (1, 0):
        lax.fori_loop(0, deep, tile, a * (1 - y) + (1 - a) * y)
        for k in turn:
            slot = 2 * k + a
            b_out[slot] = summed(k, a, 1, []).astype(jnp.bfloat16)
            push(b_out, b_in, b_recv, slot, place_b)
    for k in turn:
        a_out[k] = summed(k, 1, 0, [(b_in, b_recv, 2 * k + 1)]).astype(jnp.bfloat16)
        push(a_out, a_in, a_recv, k, place_a)
    for k in range(1, deep):
        z_out[k] = summed(k, 0, 0, [(b_in, b_recv, 2 * k), (a_in, a_recv, k)]).astype(jnp.bfloat16)
        push(z_out, z_in, z_recv, k, ((me + 4 * k) % count, core))
    arrived = [(b_in, b_recv, 0), (a_in, a_recv, 0)] + [(z_in, z_recv, k) for k in range(1, deep)]
    ffn = summed(0, 0, 0, arrived)
    finished = layer_norm(
        ALPHA * mid[...].astype(jnp.float32) + 0.5 * ffn, gain[...], shift[...]
    )
    out[core] = finished.astype(jnp.bfloat16)
    last = remote(out.at[core], out.at[core], f_sem.at[0], f_sem.at[1], twin)
    last.start()

    def drained(place, carry):
        to_twin(place).wait_send()
        return carry

    lax.fori_loop(0, count, drained, 0)
    for copy in pushed:
        copy.wait_send()
    last.wait()


def layer(local, out_gate, head_gain, out_proj, resid, mix_gain, mix_shift, sent, gain, shift):
    local_read, carry_q, own_decay, own_state = local
    count = lax.axis_size("sp")
    tok_rows, inner = resid.shape
    own = tok_rows // 2
    deep = count // 4
    states = packed_state(own_decay, own_state)
    _, slice_rows, wide = states.shape
    width = own_state.shape[-1]
    dma = pltpu.SemaphoreType.DMA
    block = lambda *lead: pltpu.VMEM((*lead, own, inner), jnp.bfloat16)
    near, far = pl.BlockSpec(memory_space=pltpu.VMEM), pl.BlockSpec(memory_space=pl.ANY)
    out = pl.pallas_call(
        functools.partial(layer_kernel, count, width),
        out_shape=jax.ShapeDtypeStruct((2, own, inner), jnp.bfloat16),
        in_specs=[near] * 5 + [far] + [near] * 3 + [far] + [near] * 2,
        out_specs=near,
        scratch_shapes=[
            pltpu.VMEM((count, slice_rows, wide), jnp.bfloat16),
            pltpu.VMEM((count, slice_rows, width), jnp.bfloat16),
            pltpu.VMEM((count, slice_rows, width), jnp.bfloat16),
            pltpu.VMEM(out_proj.shape, jnp.bfloat16),
            pltpu.VMEM((tok_rows, out_proj.shape[0]), jnp.bfloat16),
            block(2),
            block(),
            block(),
            block(2 * count),
            pltpu.VMEM((sent.shape[1], inner), jnp.bfloat16),
            block(2 * count),
            block(count),
            block(2 * deep),
            block(2 * deep),
            block(deep),
            block(deep),
            block(deep),
            block(deep),
            dma((count,)),
            dma((count,)),
            dma((count,)),
            dma((count,)),
            dma((2,)),
            dma((2 * count,)),
            dma((2 * count,)),
            dma((2 * count,)),
            dma((count,)),
            dma((count,)),
            dma((4,)),
            dma((count,)),
            dma((count,)),
            dma((count,)),
            dma((2 * deep,)),
            dma((deep,)),
            dma((deep,)),
            dma((2,)),
        ],
        compiler_params=pltpu.CompilerParams(
            collective_id=2, has_side_effects=True, vmem_limit_bytes=60 * 1024 * 1024
        ),
    )(
        states,
        local_read.reshape(tok_rows, -1),
        carry_q.reshape(tok_rows, -1),
        out_gate,
        head_gain[None],
        out_proj,
        resid.reshape(2, own, inner),
        mix_gain[None],
        mix_shift[None],
        sent,
        gain[None],
        shift[None],
    )
    return out.reshape(tok_rows, inner)


def body(
    resid,
    queries,
    keys,
    values,
    decay_pre,
    out_gate,
    head_gain,
    out_proj,
    mix_gain,
    mix_shift,
    gate_in,
    up_in,
    down_out,
    out_gain,
    out_shift,
):
    tp_count = lax.axis_size("tp")
    tok_rows = queries.shape[0]
    own_count = tok_rows // tp_count
    sp_count = lax.axis_size("sp")
    units = gate_in.shape[1]
    key_rows, heads = queries.shape[1], queries.shape[1] // HK
    by_units = (
        2 * tok_rows * sp_count < 3 * units
        and units % sp_count == 0
        and (units // sp_count) % 16 == 0
        and gate_in.shape[0] == down_out.shape[1]
        and tp_count == 2
        and sp_count % 4 == 0
        and own_count % 16 == 0
        and key_rows % (16 * sp_count) == 0
        and sp_count % heads == 0
    )
    local = local_tokens(queries, keys, values, decay_pre)
    if by_units:
        sent = own_units(gate_in, up_in, down_out)
        norms = (mix_gain, mix_shift, sent, out_gain, out_shift)
        return layer(local, out_gate, head_gain, out_proj, resid, *norms)
    gated = mix_tokens(*local, out_gate, head_gain)
    mixed = lax.psum_scatter(
        jnp.dot(gated, out_proj, preferred_element_type=jnp.float32).astype(jnp.bfloat16),
        "tp",
        scatter_dimension=0,
        tiled=True,
    ).astype(jnp.float32)
    own_resid = lax.dynamic_slice_in_dim(resid, lax.axis_index("tp") * own_count, own_count, 0)
    mid = layer_norm(ALPHA * own_resid.astype(jnp.float32) + mixed, mix_gain, mix_shift).astype(
        jnp.bfloat16
    )
    whole_rows = lax.all_gather(mid, "tp", axis=0, tiled=True)
    hidden = hidden_by_rows(whole_rows, gate_in, up_in)
    ffn = lax.psum_scatter(
        down_by_columns(hidden, down_out).astype(jnp.bfloat16),
        "tp",
        scatter_dimension=0,
        tiled=True,
    ).astype(jnp.float32)
    finished = layer_norm(ALPHA * mid.astype(jnp.float32) + 0.5 * ffn, out_gain, out_shift).astype(
        jnp.bfloat16
    )
    return lax.all_gather(finished, "tp", axis=0, tiled=True)


def solution(mesh):
    return jax.shard_map(
        body,
        mesh=mesh,
        in_specs=(
            P("sp", None),
            P("sp", "tp"),
            P("sp", "tp"),
            P("sp", "tp"),
            P("sp", "tp"),
            P("sp", "tp"),
            P(),
            P("tp", None),
            P(),
            P(),
            P("sp", "tp"),
            P("sp", "tp"),
            P("tp", "sp"),
            P(),
            P(),
        ),
        out_specs=P("sp", None),
        check_vma=False,
    )
```

```python
import functools

import jax
import jax.numpy as jnp
from jax import lax
from jax.experimental import pallas as pl
from jax.experimental.pallas import tpu as pltpu
from jax.sharding import PartitionSpec as P

HK = 128
HV = 256
SPAN = 64


ALPHA = 2.0**0.25
LN_EPS = 1e-05
RMS_EPS = 1e-06
TAU = 16.0
MESH = pl.DeviceIdType.MESH


def entering(array, axis, combine, identity):
    count, place = (lax.axis_size(axis), lax.axis_index(axis))
    everything = jax.tree.map(
        lambda part, kind: lax.all_gather(part.astype(kind), axis),
        array,
        (jnp.bfloat16, jnp.bfloat16),
    )
    start = jax.tree.map(
        lambda part, zero: jnp.broadcast_to(jnp.asarray(zero, part.dtype), part.shape),
        array,
        identity,
    )

    def lap(k, before):
        reached = k < place
        new = combine(
            before, jax.tree.map(lambda part, own: part[k].astype(own.dtype), everything, array)
        )
        return jax.tree.map(lambda a, b: jnp.where(reached, a, b), new, before)

    return lax.fori_loop(0, count, lap, start)


def layer_norm(inputs, gain, shift):
    center = inputs - jnp.mean(inputs, axis=-1, keepdims=True)
    spread = jnp.mean(center * center, axis=-1, keepdims=True)
    return center * lax.rsqrt(spread + LN_EPS) * gain + shift


def combine_states(earlier, later):
    return (earlier[0] * later[0], later[0][..., None] * earlier[1] + later[1])


def packed_state(own_decay, own_state):
    count = lax.axis_size("sp")
    rows, width = own_decay.size, own_state.shape[-1]
    decay = own_decay.reshape(count, rows // count, 1)
    high = decay.astype(jnp.bfloat16)
    low = (decay - high.astype(jnp.float32)).astype(jnp.bfloat16)
    fill = jnp.zeros((count, rows // count, 126), jnp.bfloat16)
    return jnp.concatenate(
        [own_state.reshape(count, rows // count, width).astype(jnp.bfloat16), high, low, fill],
        axis=-1,
    )


def greet(places):
    barrier = pltpu.get_barrier_semaphore()
    for place in places:
        pl.semaphore_signal(barrier, inc=1, device_id=place, device_id_type=MESH)
    pl.semaphore_wait(barrier, len(places))


def remote(src, dst, send, recv, place):
    return pltpu.make_async_remote_copy(
        src_ref=src, dst_ref=dst, send_sem=send, recv_sem=recv, device_id=place, device_id_type=MESH
    )


def local_tokens(queries, keys, values, decay_pre):
    tok_rows = queries.shape[0]
    local_heads = queries.shape[1] // HK
    blocks = tok_rows // SPAN
    logdecay = jax.nn.log_sigmoid(decay_pre) / TAU
    scaled_q = queries.astype(jnp.float32).reshape(blocks, SPAN, local_heads, HK) * HK ** (-0.5)
    key_block = keys.astype(jnp.float32).reshape(blocks, SPAN, local_heads, HK)
    value_block = values.astype(jnp.float32).reshape(blocks, SPAN, local_heads, HV)
    cumul = jnp.cumsum(logdecay.reshape(blocks, SPAN, local_heads, HK), axis=1)
    last = cumul[:, -1]
    key_decayed = key_block * jnp.exp(last[:, None] - cumul)
    updates = jnp.einsum(
        "nchk,nchv->nhkv", key_decayed, value_block, precision=lax.Precision.HIGHEST
    )

    def advance(running_state, inputs):
        decay_end, state_increment, current_query = inputs
        running_state = jnp.exp(decay_end)[..., None] * running_state + state_increment
        return (
            running_state,
            jnp.einsum(
                "qpy,pyr->qpr", current_query, running_state, precision=lax.Precision.HIGHEST
            ),
        )

    own_state, local_read = lax.scan(
        advance, jnp.zeros((local_heads, HK, HV), jnp.float32), (last, updates, scaled_q)
    )
    block_ends = jnp.cumsum(last, axis=0)
    own_decay = jnp.exp(block_ends[-1])
    carry_q = scaled_q * jnp.exp(block_ends)[:, None]
    return local_read, carry_q, own_decay, own_state


def mix_tokens(local_read, carry_q, own_decay, own_state, out_gate, head_gain):
    blocks, span, local_heads, _ = carry_q.shape
    tok_rows = blocks * span
    identity = (jnp.ones_like(own_decay), jnp.zeros_like(own_state))
    _, incoming = entering((own_decay, own_state), "sp", combine_states, identity)
    carried = jnp.einsum(
        "xepj,pjw->xepw", carry_q, incoming, precision=lax.Precision.HIGHEST
    )
    state_readout = (local_read + carried).reshape(tok_rows, local_heads, HV)
    normed = (
        state_readout
        * lax.rsqrt(jnp.mean(state_readout * state_readout, axis=-1, keepdims=True) + RMS_EPS)
        * head_gain
    )
    return (
        normed.reshape(tok_rows, local_heads * HV) * jax.nn.silu(out_gate.astype(jnp.float32))
    ).astype(jnp.bfloat16)


def hidden_by_rows(whole_rows, gate_in, up_in):
    gate = jnp.dot(
        whole_rows,
        lax.all_gather(gate_in, "sp", axis=0, tiled=True),
        preferred_element_type=jnp.float32,
    )
    upward = jnp.dot(
        whole_rows,
        lax.all_gather(up_in, "sp", axis=0, tiled=True),
        preferred_element_type=jnp.float32,
    )
    return (jax.nn.silu(gate) * upward).astype(jnp.bfloat16)


def down_by_columns(hidden, down_out):
    return jnp.dot(
        hidden,
        lax.all_gather(down_out, "sp", axis=1, tiled=True),
        preferred_element_type=jnp.float32,
    )


def own_units(gate_in, up_in, down_out):
    count = lax.axis_size("sp")
    inner, units = gate_in.shape
    piece = units // count
    sent = jnp.concatenate(
        [
            gate_in.T.reshape(count, piece, inner),
            up_in.T.reshape(count, piece, inner),
            down_out.reshape(count, piece, inner),
        ],
        axis=1,
    )
    return sent


def layer_kernel(
    count,
    width,
    states,
    local_read,
    carry_q,
    out_gate,
    head_gain,
    out_proj,
    resid,
    mix_gain,
    mix_shift,
    sent,
    gain,
    shift,
    out,
    got,
    starts,
    back,
    proj,
    gated,
    mixed,
    mixed_in,
    mid,
    rows,
    weights,
    part,
    twin_in,
    b_out,
    b_in,
    a_out,
    a_in,
    z_out,
    z_in,
    send1,
    recv1,
    send2,
    recv2,
    m_sem,
    w_send,
    w_recv,
    g_send,
    g_recv,
    t_recv,
    own_sem,
    s_send,
    p_send,
    p_recv,
    b_recv,
    a_recv,
    z_recv,
    f_sem,
):
    me, core = lax.axis_index("sp"), lax.axis_index("tp")
    deep = count // 4
    own, inner = mid.shape
    piece = sent.shape[1] // 3
    lanes = sent.shape[2]
    x, y = me % 2, (me // 2) % 2
    to_x, to_y = 1 - 2 * x, 2 - 4 * y
    to_a = (1 - core) * to_y + core * to_x
    to_b = core * to_y + (1 - core) * to_x
    place_a, place_b = (me + to_a, core), (me + to_b, core)
    twin = (me, 1 - core)
    others = [((me + j) % count, core) for j in range(1, count)]

    def spot(k, a, b):
        return (me + 4 * k) % count + a * to_a + b * to_b

    greet(others + [twin])

    moved = []
    for j, place in enumerate(others, 1):
        copy = remote(states.at[place[0]], got.at[me], send1.at[j], recv1.at[j], place)
        copy.start()
        moved.append(copy)
    columns = pl.ds(pl.multiple_of(me * lanes, lanes), lanes)
    keep = [
        pltpu.make_async_copy(states.at[me], got.at[me], own_sem.at[0]),
        pltpu.make_async_copy(out_proj, proj, own_sem.at[1]),
        pltpu.make_async_copy(sent.at[me], weights.at[:, columns], own_sem.at[2]),
    ]
    for copy in keep:
        copy.start()
    keep[0].wait()
    for copy in moved:
        copy.wait_recv()
    running = jnp.zeros(starts.shape[1:], jnp.float32)
    for k in range(count):
        starts[k] = running.astype(starts.dtype)
        if k < count - 1:
            state = got[k].astype(jnp.float32)
            decay = state[:, width : width + 1] + state[:, width + 1 : width + 2]
            running = decay * running + state[:, :width]
    returned = []
    for j, place in enumerate(others, 1):
        copy = remote(starts.at[place[0]], back.at[me], send2.at[j], recv2.at[j], place)
        copy.start()
        returned.append(copy)
    mine = pltpu.make_async_copy(starts.at[me], back.at[me], own_sem.at[3])
    mine.start()
    brought = []

    def bring(first, last):
        taken = pl.ds(first * piece, (last - first) * piece)
        for place in others:
            slot = len(brought)
            copy = remote(
                sent.at[place[0], taken],
                weights.at[taken, columns],
                w_send.at[slot],
                w_recv.at[slot],
                place,
            )
            copy.start()
            brought.append(copy)

    bring(0, 1)
    mine.wait()
    for copy in returned:
        copy.wait_recv()

    heads = gated.shape[1] // width
    key_width = carry_q.shape[1] // heads
    each = count // heads
    for h in range(heads):
        wide = slice(h * width, (h + 1) * width)
        incoming = back[h * each : (h + 1) * each].reshape(key_width, width).astype(jnp.float32)
        read = local_read[:, wide] + jnp.dot(
            carry_q[:, h * key_width : (h + 1) * key_width],
            incoming,
            precision=lax.Precision.HIGHEST,
            preferred_element_type=jnp.float32,
        )
        size = jnp.mean(read * read, axis=-1, keepdims=True)
        pre = out_gate[:, wide].astype(jnp.float32)
        normed = read * lax.rsqrt(size + RMS_EPS) * head_gain[...]
        gated[:, wide] = (normed * (pre * jax.nn.sigmoid(pre))).astype(jnp.bfloat16)
    keep[1].wait()
    summed_heads = jnp.dot(gated[...], proj[...], preferred_element_type=jnp.float32)
    mixed[...] = summed_heads.astype(jnp.bfloat16).reshape(2, own, inner)
    swap = remote(mixed.at[1 - core], mixed_in, m_sem.at[0], m_sem.at[1], twin)
    swap.start()
    swap.wait()
    total = mixed[core].astype(jnp.float32) + mixed_in[...].astype(jnp.float32)
    before = ALPHA * resid[core].astype(jnp.float32) + total
    middle = layer_norm(before, mix_gain[...], mix_shift[...]).astype(jnp.bfloat16)
    mid[...] = middle
    rows[2 * me + core] = middle

    sends = []

    def forward(k, a, b, place, slot, recv):
        block = 2 * spot(k, a, b) + core
        src = mid if (k, a, b) == (0, 0, 0) else rows.at[block]
        copy = remote(src, rows.at[block], g_send.at[len(sends)], recv.at[slot], place)
        copy.start()
        sends.append(copy)

    def index(k, a, b):
        return (k * 2 + a) * 2 + b

    def landed(k, a, b):
        block = rows.at[2 * spot(k, a, b) + core]
        remote(block, block, g_send.at[0], g_recv.at[index(k, a, b)], twin).wait_recv()

    def onward(k, a, b):
        if not b:
            if not a:
                forward(k, 0, 0, place_a, index(k, 1, 0), g_recv)
            forward(k, a, 0, place_b, index(k, a, 1), g_recv)
        forward(k, a, b, twin, index(k, b, a), t_recv)

    for k in range(1, deep):
        forward(0, 0, 0, ((me + 4 * k) % count, core), index(deep - k, 0, 0), g_recv)
    onward(0, 0, 0)
    bring(1, 2)
    order = [(0, 1, 0)] + [(k, 0, 0) for k in range(1, deep)]
    order += [(k, 1, 0) for k in range(1, deep)]
    order += [(k, a, 1) for k in range(deep) for a in range(2)]
    for block in order:
        landed(*block)
        onward(*block)
        if block == (deep - 1, 0, 0):
            bring(2, 3)
    for k in range(deep):
        for a in range(2):
            for b in range(2):
                block = rows.at[2 * spot(k, b, a) + 1 - core]
                remote(block, block, g_send.at[0], t_recv.at[index(k, a, b)], twin).wait_recv()
    keep[2].wait()
    for copy in brought:
        copy.wait_recv()
    for copy in sends + moved + returned + brought:
        copy.wait_send()

    contract = (((1,), (1,)), ((), ()))

    def to_twin(place):
        return remote(
            part.at[2 * place + 1 - core],
            twin_in.at[place],
            p_send.at[place],
            p_recv.at[place],
            twin,
        )

    def tile(step, side):
        i = 2 * ((me // 4 + step) % deep) + side
        left = rows[pl.ds(4 * i, 4)].reshape(4 * own, inner)
        gate = lax.dot_general(left, weights[:piece], contract, preferred_element_type=jnp.float32)
        up = lax.dot_general(
            left, weights[piece : 2 * piece], contract, preferred_element_type=jnp.float32
        )
        hidden = (gate * jax.nn.sigmoid(gate) * up).astype(jnp.bfloat16)
        down = jnp.dot(hidden, weights[2 * piece :], preferred_element_type=jnp.float32)
        part[pl.ds(4 * i, 4)] = down.astype(jnp.bfloat16).reshape(4, own, inner)
        to_twin(2 * i).start()
        to_twin(2 * i + 1).start()
        return side

    def summed(k, a, b, arrived):
        place = spot(k, a, b)
        to_twin(place).wait_recv()
        total = part[2 * place + core].astype(jnp.float32) + twin_in[place].astype(jnp.float32)
        for ref, sem, slot in arrived:
            remote(ref.at[slot], ref.at[slot], s_send.at[0], sem.at[slot], twin).wait_recv()
            total = total + ref[slot].astype(jnp.float32)
        return total

    pushed = []

    def push(src, dst, recv, slot, place):
        copy = remote(src.at[slot], dst.at[slot], s_send.at[len(pushed)], recv.at[slot], place)
        copy.start()
        pushed.append(copy)

    turn = [k for k in range(1, deep)] + [0]
    for a in (1, 0):
        lax.fori_loop(0, deep, tile, a * (1 - y) + (1 - a) * y)
        for k in turn:
            slot = 2 * k + a
            b_out[slot] = summed(k, a, 1, []).astype(jnp.bfloat16)
            push(b_out, b_in, b_recv, slot, place_b)
    for k in turn:
        a_out[k] = summed(k, 1, 0, [(b_in, b_recv, 2 * k + 1)]).astype(jnp.bfloat16)
        push(a_out, a_in, a_recv, k, place_a)
    for k in range(1, deep):
        z_out[k] = summed(k, 0, 0, [(b_in, b_recv, 2 * k), (a_in, a_recv, k)]).astype(jnp.bfloat16)
        push(z_out, z_in, z_recv, k, ((me + 4 * k) % count, core))
    arrived = [(b_in, b_recv, 0), (a_in, a_recv, 0)] + [(z_in, z_recv, k) for k in range(1, deep)]
    ffn = summed(0, 0, 0, arrived)
    finished = layer_norm(
        ALPHA * mid[...].astype(jnp.float32) + 0.5 * ffn, gain[...], shift[...]
    )
    out[core] = finished.astype(jnp.bfloat16)
    last = remote(out.at[core], out.at[core], f_sem.at[0], f_sem.at[1], twin)
    last.start()

    def drained(place, carry):
        to_twin(place).wait_send()
        return carry

    lax.fori_loop(0, count, drained, 0)
    for copy in pushed:
        copy.wait_send()
    last.wait()


def layer(local, out_gate, head_gain, out_proj, resid, mix_gain, mix_shift, sent, gain, shift):
    local_read, carry_q, own_decay, own_state = local
    count = lax.axis_size("sp")
    tok_rows, inner = resid.shape
    own = tok_rows // 2
    deep = count // 4
    states = packed_state(own_decay, own_state)
    _, slice_rows, wide = states.shape
    width = own_state.shape[-1]
    dma = pltpu.SemaphoreType.DMA
    block = lambda *lead: pltpu.VMEM((*lead, own, inner), jnp.bfloat16)
    near, far = pl.BlockSpec(memory_space=pltpu.VMEM), pl.BlockSpec(memory_space=pl.ANY)
    out = pl.pallas_call(
        functools.partial(layer_kernel, count, width),
        out_shape=jax.ShapeDtypeStruct((2, own, inner), jnp.bfloat16),
        in_specs=[near] * 5 + [far] + [near] * 3 + [far] + [near] * 2,
        out_specs=near,
        scratch_shapes=[
            pltpu.VMEM((count, slice_rows, wide), jnp.bfloat16),
            pltpu.VMEM((count, slice_rows, width), jnp.bfloat16),
            pltpu.VMEM((count, slice_rows, width), jnp.bfloat16),
            pltpu.VMEM(out_proj.shape, jnp.bfloat16),
            pltpu.VMEM((tok_rows, out_proj.shape[0]), jnp.bfloat16),
            block(2),
            block(),
            block(),
            block(2 * count),
            pltpu.VMEM((sent.shape[1], inner), jnp.bfloat16),
            block(2 * count),
            block(count),
            block(2 * deep),
            block(2 * deep),
            block(deep),
            block(deep),
            block(deep),
            block(deep),
            dma((count,)),
            dma((count,)),
            dma((count,)),
            dma((count,)),
            dma((2,)),
            dma((3 * count,)),
            dma((3 * count,)),
            dma((2 * count,)),
            dma((count,)),
            dma((count,)),
            dma((4,)),
            dma((count,)),
            dma((count,)),
            dma((count,)),
            dma((2 * deep,)),
            dma((deep,)),
            dma((deep,)),
            dma((2,)),
        ],
        compiler_params=pltpu.CompilerParams(
            collective_id=2, has_side_effects=True, vmem_limit_bytes=60 * 1024 * 1024
        ),
    )(
        states,
        local_read.reshape(tok_rows, -1),
        carry_q.reshape(tok_rows, -1),
        out_gate,
        head_gain[None],
        out_proj,
        resid.reshape(2, own, inner),
        mix_gain[None],
        mix_shift[None],
        sent,
        gain[None],
        shift[None],
    )
    return out.reshape(tok_rows, inner)


def body(
    resid,
    queries,
    keys,
    values,
    decay_pre,
    out_gate,
    head_gain,
    out_proj,
    mix_gain,
    mix_shift,
    gate_in,
    up_in,
    down_out,
    out_gain,
    out_shift,
):
    tp_count = lax.axis_size("tp")
    tok_rows = queries.shape[0]
    own_count = tok_rows // tp_count
    sp_count = lax.axis_size("sp")
    units = gate_in.shape[1]
    key_rows, heads = queries.shape[1], queries.shape[1] // HK
    by_units = (
        2 * tok_rows * sp_count < 3 * units
        and units % sp_count == 0
        and (units // sp_count) % 16 == 0
        and gate_in.shape[0] == down_out.shape[1]
        and tp_count == 2
        and sp_count % 4 == 0
        and own_count % 16 == 0
        and key_rows % (16 * sp_count) == 0
        and sp_count % heads == 0
    )
    local = local_tokens(queries, keys, values, decay_pre)
    if by_units:
        sent = own_units(gate_in, up_in, down_out)
        norms = (mix_gain, mix_shift, sent, out_gain, out_shift)
        return layer(local, out_gate, head_gain, out_proj, resid, *norms)
    gated = mix_tokens(*local, out_gate, head_gain)
    mixed = lax.psum_scatter(
        jnp.dot(gated, out_proj, preferred_element_type=jnp.float32).astype(jnp.bfloat16),
        "tp",
        scatter_dimension=0,
        tiled=True,
    ).astype(jnp.float32)
    own_resid = lax.dynamic_slice_in_dim(resid, lax.axis_index("tp") * own_count, own_count, 0)
    mid = layer_norm(ALPHA * own_resid.astype(jnp.float32) + mixed, mix_gain, mix_shift).astype(
        jnp.bfloat16
    )
    whole_rows = lax.all_gather(mid, "tp", axis=0, tiled=True)
    hidden = hidden_by_rows(whole_rows, gate_in, up_in)
    ffn = lax.psum_scatter(
        down_by_columns(hidden, down_out).astype(jnp.bfloat16),
        "tp",
        scatter_dimension=0,
        tiled=True,
    ).astype(jnp.float32)
    finished = layer_norm(ALPHA * mid.astype(jnp.float32) + 0.5 * ffn, out_gain, out_shift).astype(
        jnp.bfloat16
    )
    return lax.all_gather(finished, "tp", axis=0, tiled=True)


def solution(mesh):
    return jax.shard_map(
        body,
        mesh=mesh,
        in_specs=(
            P("sp", None),
            P("sp", "tp"),
            P("sp", "tp"),
            P("sp", "tp"),
            P("sp", "tp"),
            P("sp", "tp"),
            P(),
            P("tp", None),
            P(),
            P(),
            P("sp", "tp"),
            P("sp", "tp"),
            P("tp", "sp"),
            P(),
            P(),
        ),
        out_specs=P("sp", None),
        check_vma=False,
    )
```
